512 devices in a mesh: ep: 128 (over z, x, core), tp: 4 (over y).
Axes of the slice: x: 4, y: 4, z: 16, core: 2. Of those that a mesh axis runs over, the one named last changes fastest.
Arguments:
- tokens: bfloat16 [16384, 2048], P('ep'), may hold values from -6 to 6
- norm_gain: float32 [2048], replicated, may hold values from 0.1 to 1.9
- expert_ids: int32 [16384, 2], P('ep'), may hold values from 0 to 31, all different within a row; in each aligned block of 128 rows (0 to 127, 128 to 255, ...) at most 12 rows name the same one
- gate_weights: float32 [16384, 2], P('ep'), may hold values from 0.2 to 1
- w_gate: bfloat16 [2048, 131072], P(None, ('ep', 'tp')), may hold values from -0.125 to 0.125
- w_up: bfloat16 [2048, 131072], P(None, ('ep', 'tp')), may hold values from -0.125 to 0.125
- w_down: bfloat16 [131072, 2048], P('ep', 'tp'), may hold values from -0.09375 to 0.09375
Outputs:
- moe_out: bfloat16 [16384, 2048], P('ep', 'tp')
The draws below stay inside these ranges and needn't reach their ends.
Inputs may be any that keep to these rules, and one draw needn't show every extreme that they name: `expert_ids`: each token names 2 different experts; in each aligned block of 128 rows no expert is named by more than 12 rows, a bound that some block reaches.
All inputs are finite; a program needn't handle non-finite values.
Results may differ from the reference program's by a relative error of at most 0.0071.
Values may be sent and summed in bfloat16 or wider, within the bound.
A program may use at most 64 MiB of HBM per device.

```python
import math
import jax
import jax.numpy as jnp
import numpy as np
from jax import lax

D = 2048
FF = 4096
TOP = 2
TOK_DEV = 128
GROUP = 4
EXPERTS = 32
CAP = 12
TOKENS = 16384
N_EP = 128


def levels(own_key, shape, pieces, smallest, largest):
    level = 1.0
    for axis_at, parts in pieces:
        heights = jax.random.uniform(jax.random.fold_in(jax.random.fold_in(own_key, 6), axis_at), (parts,), jnp.float32, smallest / len(pieces), largest / len(pieces))
        level = level * jnp.repeat(jnp.exp(heights), shape[axis_at] // parts).reshape((-1,) + (1,) * (len(shape) - 1 - axis_at))
    return level


def assign_block(key, own, number, rows, count, top, reach, slope):
    order = jax.random.permutation(key, count)
    packed, ordinary = load_shares(count, rows * top, reach, slope, True), load_shares(count, rows * top, reach, slope, False)
    places = jnp.arange(count)

    def named(lengths, rotation):
        used = int((lengths > 0).sum())
        fixed = max(1, used // 4)
        moved = fixed + (places - fixed + rotation * (used - fixed)) % max(1, count - fixed)
        return jnp.zeros((count,), jnp.int32).at[order[jnp.where(places < fixed, places, moved)]].set(jnp.asarray(lengths, jnp.int32))

    lengths = jnp.where(number % 4 == 0, named(packed, number // 4), named(ordinary, number - number // 4 - 1))
    mixed = jax.random.permutation(jax.random.fold_in(own, 3), count)
    giver, receiver = mixed[0:count // 2 * 2:2], mixed[1:count // 2 * 2:2]
    margin = jnp.minimum(lengths[giver] - 1, reach - lengths[receiver]) // 2
    margin = jnp.where((giver == order[0]) | (receiver == order[0]) | (lengths[receiver] == 0), 0, jnp.maximum(margin, 0))
    moved = jax.random.randint(jax.random.fold_in(own, 4), (count // 2,), 0, 1 << 20) % (margin + 1)
    lengths = lengths.at[giver].add(-moved).at[receiver].add(moved)
    items = jnp.searchsorted(jnp.cumsum(lengths), jnp.arange(rows * top), side="right").astype(jnp.int32)
    table = items.reshape(top, rows).T
    table = table[jax.random.permutation(jax.random.fold_in(own, 1), rows)]
    rotation = jax.random.randint(jax.random.fold_in(own, 2), (rows, 1), 0, top)
    return jnp.take_along_axis(table, (jnp.arange(top)[None, :] + rotation) % top, axis=1)


def load_shares(number_of, total, limit, skew, full):
    loads = [(1 << 20) // math.isqrt(grade ** skew) + 1 for grade in range(1, number_of + 1)]
    largest = limit if full else min(limit, max(-(-total // number_of), total * loads[0] // sum(loads)))
    least = 1 if total - largest >= number_of - 1 else 0
    counts, rest = [largest] + [least] * (number_of - 1), total - largest - least * (number_of - 1)
    while rest > 0:
        free = [i for i in range(1, number_of) if counts[i] < largest] or [i for i in range(1, number_of) if counts[i] < limit]
        mass, remaining = sum([loads[i] for i in free]), rest
        for i in free:
            more = min(limit - counts[i], max(1, remaining * loads[i] // mass), rest)
            counts[i] = counts[i] + more
            rest = rest - more
    return np.array(counts)


def noise(own_key, shape, deviation, limit, cuts=(), held_as=jnp.bfloat16):
    values = deviation * jax.random.normal(own_key, shape, jnp.float32)
    if cuts:
        values = values * levels(own_key, shape, cuts, -0.22, 0.18)
    return jnp.clip(values, -limit, limit).astype(held_as)


def setup_inputs(seed: int = 0) -> dict:
    key_of = jax.random.split(jax.random.key(seed), 8)
    tokens = noise(key_of[0], (TOKENS, D), 1.0, 6.0, ((0, 128),))
    norm_gain = jnp.clip(1.0 + 0.18 * jax.random.normal(key_of[1], (D,), jnp.float32), 0.1, 1.9)
    expert_ids_keys = jax.random.split(jax.random.fold_in(key_of[2], 1), TOKENS // TOK_DEV)
    expert_ids_turns = jax.random.permutation(jax.random.fold_in(key_of[2], 3), TOKENS // TOK_DEV)
    expert_ids = jax.vmap(lambda own, number: assign_block(jax.random.fold_in(key_of[2], 2), own, number, TOK_DEV, EXPERTS, TOP, CAP, 2))(expert_ids_keys, expert_ids_turns).reshape((TOKENS, TOP))
    gate_weights = jnp.clip(0.2 + 0.8 * jax.random.uniform(key_of[3], (TOKENS, TOP), jnp.float32) ** levels(key_of[3], (TOKENS, TOP), ((0, 128),), -0.2, 0.2), 0.2, 1.0)
    w_gate = noise(key_of[4], (D, EXPERTS * FF), D ** -0.5, 0.125, ((1, 512),))
    w_up = noise(key_of[5], (D, EXPERTS * FF), D ** -0.5, 0.125, ((1, 512),))
    w_down = noise(key_of[6], (EXPERTS * FF, D), FF ** -0.5, 0.09375, ((0, 128), (1, 4)))
    return {"tokens": tokens, "norm_gain": norm_gain, "expert_ids": expert_ids, "gate_weights": gate_weights, "w_gate": w_gate, "w_up": w_up, "w_down": w_down}


EPS = 1e-06

def rms_rows(values, gain):
    widened = values.astype(jnp.float32)
    scale = lax.rsqrt(lax.optimization_barrier(jnp.mean(widened * widened, axis=-1, keepdims=True)) + EPS)
    return (widened * scale * gain).astype(jnp.bfloat16)

def reference(tokens, norm_gain, expert_ids, gate_weights, w_gate, w_up, w_down):
    normed = rms_rows(tokens, norm_gain)
    block_width = FF // GROUP
    slots_most = min(CAP * N_EP, TOKENS)
    flat_ids = expert_ids.reshape(-1).astype(jnp.int32)
    flat_gates = gate_weights.reshape(-1).astype(jnp.float32)
    owners = (jnp.arange(TOKENS * TOP, dtype=jnp.int32) // TOP).astype(jnp.int32)

    def one_expert(expert, output):
        matches = (flat_ids == expert).astype(jnp.int32)
        ranks = (jnp.cumsum(matches) - matches).astype(jnp.int32)
        target = jnp.where(matches == 1, ranks, slots_most).astype(jnp.int32)
        sources = jnp.zeros((slots_most,), jnp.int32).at[target].set(owners, mode='drop')
        scales = jnp.zeros((slots_most,), jnp.float32).at[target].set(flat_gates, mode='drop')
        picked = normed[sources]
        gate_cols = lax.dynamic_slice_in_dim(w_gate, expert * FF, FF, 1)
        up_cols = lax.dynamic_slice_in_dim(w_up, expert * FF, FF, 1)
        down_rows = lax.dynamic_slice_in_dim(w_down, expert * FF, FF, 0)
        gate_proj = jnp.dot(picked, gate_cols, preferred_element_type=jnp.float32)
        upper = jnp.dot(picked, up_cols, preferred_element_type=jnp.float32)
        hidden = (jax.nn.silu(gate_proj) * upper).astype(jnp.bfloat16)

        def add_block(block, total):
            piece = lax.dynamic_slice_in_dim(hidden, block * block_width, block_width, 1)
            weights = lax.dynamic_slice_in_dim(down_rows, block * block_width, block_width, 0)
            partial_out = jnp.dot(piece, weights, preferred_element_type=jnp.float32).astype(jnp.bfloat16)
            partial_out = lax.optimization_barrier(partial_out)
            return total + partial_out.astype(jnp.float32)
        total = lax.fori_loop(0, GROUP, add_block, jnp.zeros((slots_most, D), jnp.float32))
        return output.at[sources].add(total * scales[:, None])
    output = lax.fori_loop(0, EXPERTS, one_expert, jnp.zeros((TOKENS, D), jnp.float32))
    return output.astype(jnp.bfloat16)
```

```python
import functools

import jax
import jax.numpy as jnp
from jax import lax
from jax.experimental import pallas as pl
from jax.experimental.pallas import tpu as pltpu
from jax.sharding import Mesh
from jax.sharding import PartitionSpec as P

MESH = pl.DeviceIdType.MESH
EP = ("z", "x", "core")
EPS = 1e-06
XN = 4
CN = 2
YN = 4
K3 = 3
CAP = YN * K3
NEAR_FIRST = ((0, 1, -1, 2), (8, 7, -7, -6), (6, 5, -5, -4), (4, 3, -3, -2))

BF16 = jnp.bfloat16
F32 = jnp.float32


def chunks_of(zn):
    return NEAR_FIRST if zn == 16 else tuple((d,) for d in range(zn))


def when(stage, c):
    base = (5.0 * c, 5.0 * c + 3.0, 5.0 * c + 6.0, 8.3 * c + 12.0, 8.3 * c + 18.0, 8.3 * c + 22.0, 8.3 * c + 27.0)
    return base[stage]


def kernel(
    zn,
    tokens,
    gain,
    ids,
    gates,
    w_gate,
    w_up,
    w_down,
    out,
    sbuf,
    xb,
    fb,
    xr,
    hb,
    wgv,
    wuv,
    wdv,
    pf,
    pb,
    rsb,
    gb,
    rb,
    ret,
    vb,
    wl_sem,
    ws_sem,
    wr_sem,
    ds_sem,
    dr_sem,
    ys_sem,
    yr_sem,
    xs_sem,
    xr_sem,
    hs_sem,
    hr_sem,
    rs_sem,
    rr_sem,
    os_sem,
    or_sem,
):
    zc, xc, cc, yc = (lax.axis_index(a) for a in ("z", "x", "core", "tp"))
    chunks = chunks_of(zn)
    offsets = [d for chunk in chunks for d in chunk]
    messages = 2 * len(offsets)
    starts = [0]
    for chunk in chunks:
        starts.append(starts[-1] + 2 * len(chunk))
    row_count, width = tokens.shape
    pieces = width // 128
    units = w_gate.shape[1]
    out_pieces = w_down.shape[1] // 128

    other_x = XN - 1 - xc
    pair_x = xc + 1 - 2 * lax.rem(xc, 2)
    up_y, down_y = lax.rem(yc + 1, YN), lax.rem(yc + YN - 1, YN)
    sibling = (zc, xc, 1 - cc, yc)
    pair = (zc, pair_x, cc, yc)
    sides = ((zc, xc, cc, up_y), (zc, xc, cc, down_y))

    def far(m, sign):
        d = offsets[m // 2] * sign
        return (lax.rem(zc + d + zn, zn), xc if m % 2 == 0 else other_x, cc, yc)

    self_message = 2 * offsets.index(0)

    barrier = pltpu.get_barrier_semaphore()
    greeted = [far(m, 1) for m in range(messages) if m != self_message] + [sibling, pair, *sides]
    for device in greeted:
        pl.semaphore_signal(barrier, inc=1, device_id=device, device_id_type=MESH)

    weights = ((w_gate, wgv), (w_up, wuv), (w_down, wdv))
    own_weights = [pltpu.make_async_copy(src, dst.at[0], wl_sem.at[i]) for i, (src, dst) in enumerate(weights)]
    for copy in own_weights:
        copy.start()

    wide = tokens[...].astype(F32)
    scale = lax.rsqrt(jnp.mean(wide * wide, axis=-1, keepdims=True) + EPS)
    normed = (wide * scale * gain[...]).astype(BF16)

    earlier = (
        lax.broadcasted_iota(jnp.int32, (row_count, row_count), 1)
        < lax.broadcasted_iota(jnp.int32, (row_count, row_count), 0)
    ).astype(F32).astype(BF16)
    first_id, second_id = ids[:, 0:1], ids[:, 1:2]

    def expert_of(message):
        expert = jnp.zeros_like(message) - 1
        for m in range(messages):
            z, x, _, _ = far(m, 1)
            expert = jnp.where(message == m, z * (XN // 2) + x // 2, expert)
        return expert

    def selection(message, slot):
        expert = expert_of(message)
        hit_first, hit_second = first_id == expert, second_id == expert
        hit = jnp.where(hit_first | hit_second, 1.0, 0.0)
        rank = jnp.dot(earlier, hit.astype(BF16), preferred_element_type=F32)
        taken = jnp.where(rank == slot.astype(F32), hit, 0.0)
        return taken, hit_first

    lane = lax.broadcasted_iota(jnp.int32, (1, 128), 1)
    taken, _ = selection(lane // K3, K3 * yc + lane % K3)
    sent_rows = messages * K3
    placed = jnp.dot(jnp.transpose(taken).astype(BF16), normed, preferred_element_type=F32)
    for i in range(pieces):
        fb[pl.ds(i, sent_rows, stride=pieces), :] = placed[:sent_rows, i * 128 : (i + 1) * 128]
    sbuf[...] = fb[0 : sent_rows * pieces, :].reshape(sent_rows, pieces, 128).astype(BF16)
    xb[0, yc, self_message * K3 : (self_message + 1) * K3] = sbuf[self_message * K3 : (self_message + 1) * K3]

    pl.semaphore_wait(barrier, len(greeted))

    sends = []

    def remote(src, dst, send_sem, recv_sem, device, later=True):
        copy = pltpu.make_async_remote_copy(
            src_ref=src, dst_ref=dst, send_sem=send_sem, recv_sem=recv_sem, device_id=device, device_id_type=MESH
        )
        copy.start()
        if later:
            sends.append(copy)
        return copy

    def arrived(ref, sem):
        pltpu.make_async_copy(ref, ref, sem).wait()

    def without_self(c):
        m0, m1 = starts[c], starts[c + 1]
        if not m0 <= self_message < m1:
            return (m0, m1)
        assert self_message == m0
        return (m0 + 1, m1)

    for c in range(len(chunks)):
        for m in range(*without_self(c)):
            rows = pl.ds(m * K3, K3)
            remote(sbuf.at[rows], xb.at[0, yc, rows], ds_sem.at[c], dr_sem.at[c], far(m, 1), later=False)
    shared_weights = [
        remote(src, dst.at[1], ws_sem.at[i], wr_sem.at[i], sibling) for i, (src, dst) in enumerate(weights)
    ]

    lane = lax.broadcasted_iota(jnp.int32, (1, messages * CAP), 1)
    taken, hit_first = selection(lane // CAP, lane % CAP)
    mix = taken * jnp.where(hit_first, gates[:, 0:1], gates[:, 1:2])

    def run(c):
        m0, m1 = starts[c], starts[c + 1]
        return pl.ds(m0 * K3, (m1 - m0) * K3)

    def half(c, side):
        m0, m1 = starts[c], starts[c + 1]
        count = (m1 - m0) // 2 * K3
        return pl.ds(m0 * K3 + side * count, count)

    origin = [lax.rem(yc - r + YN, YN) for r in range(YN)]
    handles = {}

    def own_rows(c):
        m0, m1 = without_self(c)
        rows = pl.ds(m0 * K3, (m1 - m0) * K3)
        arrived(xb.at[0, yc, rows], dr_sem.at[c])
        block = xb.at[0, yc, run(c)]
        for side in (0, 1):
            handles["y", c, side] = remote(
                block, block, ys_sem.at[c, side], yr_sem.at[c, side], sides[side]
            )
        handles["x", c, 0] = remote(block, xb.at[1, yc, run(c)], xs_sem.at[c, 0], xr_sem.at[c, 0], pair)

    def next_rows(c):
        for side in (0, 1):
            handles["y", c, side].wait_recv()
            rel = 1 + 2 * side
            part = xb.at[0, origin[rel], half(c, side)]
            handles["f", c, side] = remote(
                part,
                part,
                ys_sem.at[c, 2 + side],
                yr_sem.at[c, 2 + side],
                sides[side],
            )
            handles["x", c, rel] = remote(
                xb.at[0, origin[rel], run(c)],
                xb.at[1, origin[rel], run(c)],
                xs_sem.at[c, rel],
                xr_sem.at[c, rel],
                pair,
            )

    def last_rows(c):
        for side in (0, 1):
            handles["f", c, side].wait_recv()
        handles["x", c, 2] = remote(
            xb.at[0, origin[2], run(c)], xb.at[1, origin[2], run(c)], xs_sem.at[c, 2], xr_sem.at[c, 2], pair
        )

    def chunk_rows(c):
        count = 2 * CAP * (starts[c + 1] - starts[c])
        return 2 * CAP * starts[c], count

    def first_product(c):
        for rel in range(YN):
            handles["x", c, rel].wait_recv()
        if c == 0:
            for copy in own_weights:
                copy.wait()
            for copy in shared_weights:
                copy.wait_recv()
        r0, count = chunk_rows(c)
        m0, m1 = starts[c], starts[c + 1]
        for side in (0, 1):
            for m in range(m0, m1):
                for y in range(YN):
                    at = ((side * (m1 - m0) + m - m0) * CAP + y * K3) * pieces
                    block = xb[side, y, m * K3 : (m + 1) * K3].astype(F32)
                    fb[at : at + K3 * pieces, :] = block.reshape(K3 * pieces, 128)
        for i in range(pieces):
            xr[0:count, i * 128 : (i + 1) * 128] = fb[pl.ds(i, count, stride=pieces), :].astype(BF16)
        for core in range(CN):
            gate = jnp.dot(xr[0:count, :], wgv[core], preferred_element_type=F32)
            upper = jnp.dot(xr[0:count, :], wuv[core], preferred_element_type=F32)
            hidden = gate / (1.0 + jnp.exp(-gate)) * upper
            hb[0, r0 : r0 + count, core * units : (core + 1) * units] = hidden.astype(BF16)
        for side in (0, 1):
            handles["h", c, side] = remote(
                hb.at[0, pl.ds(r0, count)],
                hb.at[1 + 2 * side, pl.ds(r0, count)],
                hs_sem.at[c, side],
                hr_sem.at[c, side],
                sides[side],
            )

    def next_hidden(c):
        r0, count = chunk_rows(c)
        for side in (0, 1):
            handles["h", c, side].wait_recv()
            rows = pl.ds(r0 + side * (count // 2), count // 2)
            handles["k", c, side] = remote(
                hb.at[1 + 2 * side, rows],
                hb.at[2, rows],
                hs_sem.at[c, 2 + side],
                hr_sem.at[c, 2 + side],
                sides[side],
            )

    def second_product(c):
        for side in (0, 1):
            handles["k", c, side].wait_recv()
        r0, count = chunk_rows(c)
        total = None
        for rel in range(YN):
            first = pl.multiple_of(origin[rel] * units, units)
            for core in range(CN):
                term = jnp.dot(
                    hb[rel, r0 : r0 + count, core * units : (core + 1) * units],
                    wdv[core, pl.ds(first, units), :],
                    preferred_element_type=F32,
                )
                total = term if total is None else total + term
        at, part = r0 // 2, count // 2
        pf[at : at + part, :] = total[0:part]
        pb[at : at + part, :] = total[part:count].astype(BF16)
        handles["r", c] = remote(
            pb.at[pl.ds(at, part)], rsb.at[pl.ds(at, part)], rs_sem.at[c], rr_sem.at[c], pair
        )

    def give_back(c):
        handles["r", c].wait_recv()
        r0, count = chunk_rows(c)
        at, part = r0 // 2, count // 2
        total = pf[at : at + part, :] + rsb[at : at + part, :].astype(F32)
        for i in range(out_pieces):
            gb[pl.ds(i, part, stride=out_pieces), :] = total[:, i * 128 : (i + 1) * 128]
        rb[at * out_pieces : (at + part) * out_pieces, :] = gb[0 : part * out_pieces, :].astype(BF16)
        size = CAP * out_pieces
        m0, m1 = starts[c], starts[c + 1]
        if m0 <= self_message < m1:
            ret[self_message * size : (self_message + 1) * size, :] = rb[
                self_message * size : (self_message + 1) * size, :
            ]
        for m in range(*without_self(c)):
            rows = pl.ds(m * size, size)
            remote(rb.at[rows], ret.at[rows], os_sem.at[c], or_sem.at[c], far(m, -1), later=False)

    stages = (own_rows, next_rows, last_rows, first_product, next_hidden, second_product, give_back)
    order = sorted((when(s, c), c, s) for c in range(len(chunks)) for s in range(len(stages)))
    for _, c, s in order:
        stages[s](c)

    size = CAP * out_pieces
    for c in range(len(chunks)):
        m0, m1 = without_self(c)
        arrived(ret.at[pl.ds(m0 * size, (m1 - m0) * size)], or_sem.at[c])
    gb[0 : messages * size, :] = ret[...].astype(F32)
    for i in range(out_pieces):
        vb[:, i * 128 : (i + 1) * 128] = gb[pl.ds(i, messages * CAP, stride=out_pieces), :].astype(BF16)
    values = vb[...]
    high = mix.astype(BF16)
    rest = mix - high.astype(F32)
    middle = rest.astype(BF16)
    low = (rest - middle.astype(F32)).astype(BF16)
    mixed = jnp.dot(high, values, preferred_element_type=F32)
    mixed = mixed + jnp.dot(middle, values, preferred_element_type=F32)
    mixed = mixed + jnp.dot(low, values, preferred_element_type=F32)
    out[...] = mixed.astype(BF16)

    for copy in sends:
        copy.wait_send()
    for c in range(len(chunks)):
        m0, m1 = without_self(c)
        arrived(sbuf.at[pl.ds(m0 * K3, (m1 - m0) * K3)], ds_sem.at[c])
        arrived(rb.at[pl.ds(m0 * size, (m1 - m0) * size)], os_sem.at[c])


def on_device(zn, tokens, norm_gain, expert_ids, gate_weights, w_gate, w_up, w_down):
    chunks = chunks_of(zn)
    n = len(chunks)
    messages = 2 * sum(len(chunk) for chunk in chunks)
    most = 2 * max(len(chunk) for chunk in chunks)
    row_count, width = tokens.shape
    pieces = width // 128
    units = w_gate.shape[1]
    block, columns = w_down.shape
    out_pieces = columns // 128
    rows = messages * CAP
    dma = pltpu.SemaphoreType.DMA
    scratch = [
        pltpu.VMEM((messages * K3, pieces, 128), BF16),
        pltpu.VMEM((2, YN, messages * K3, pieces, 128), BF16),
        pltpu.VMEM((max(2 * most * CAP, messages * K3) * pieces, 128), F32),
        pltpu.VMEM((2 * most * CAP, width), BF16),
        pltpu.VMEM((YN, 2 * rows, CN * units), BF16),
        pltpu.VMEM((CN, width, units), BF16),
        pltpu.VMEM((CN, width, units), BF16),
        pltpu.VMEM((CN, block, columns), BF16),
        pltpu.VMEM((rows, columns), F32),
        pltpu.VMEM((rows, columns), BF16),
        pltpu.VMEM((rows, columns), BF16),
        pltpu.VMEM((rows * out_pieces, 128), F32),
        pltpu.VMEM((rows * out_pieces, 128), BF16),
        pltpu.VMEM((rows * out_pieces, 128), BF16),
        pltpu.VMEM((rows, columns), BF16),
        dma((3,)),
        dma((3,)),
        dma((3,)),
        dma((n,)),
        dma((n,)),
        dma((n, 4)),
        dma((n, 4)),
        dma((n, 4)),
        dma((n, 4)),
        dma((n, 4)),
        dma((n, 4)),
        dma((n,)),
        dma((n,)),
        dma((n,)),
        dma((n,)),
    ]
    vmem = pl.BlockSpec(memory_space=pltpu.VMEM)
    hbm = pl.BlockSpec(memory_space=pl.ANY)
    return pl.pallas_call(
        functools.partial(kernel, zn),
        out_shape=jax.ShapeDtypeStruct((row_count, columns), BF16),
        in_specs=[vmem, vmem, vmem, vmem, hbm, hbm, hbm],
        out_specs=vmem,
        scratch_shapes=scratch,
        compiler_params=pltpu.CompilerParams(
            collective_id=0, has_side_effects=True, vmem_limit_bytes=60 * 1024 * 1024
        ),
        name="expert_layer",
    )(tokens, norm_gain.reshape(1, width), expert_ids, gate_weights, w_gate, w_up, w_down)


def solution(mesh):
    zn = mesh.shape["ep"] // (XN * CN)
    finer = Mesh(mesh.devices.reshape(zn, XN, CN, mesh.shape["tp"]), (*EP, "tp"))
    placed = (
        P(EP, None),
        P(),
        P(EP, None),
        P(EP, None),
        P(None, (*EP, "tp")),
        P(None, (*EP, "tp")),
        P(EP, "tp"),
    )
    return jax.shard_map(
        functools.partial(on_device, zn), mesh=finer, in_specs=placed, out_specs=P(EP, "tp"), check_vma=False
    )
```

```python
import functools

import jax
import jax.numpy as jnp
from jax import lax
from jax.experimental import pallas as pl
from jax.experimental.pallas import tpu as pltpu
from jax.sharding import Mesh
from jax.sharding import PartitionSpec as P

MESH = pl.DeviceIdType.MESH
EP = ("z", "x", "core")
EPS = 1e-06
XN = 4
CN = 2
YN = 4
K3 = 3
CAP = YN * K3
CHUNKS = ((-1, 1), (5, -5), (6, -6), (2, -2), (-7, 7), (8, 0), (-4, 4), (-3, 3))
ORDER = "00101312032412641352460762541325746132754673405637567570"

BF16 = jnp.bfloat16
F32 = jnp.float32


def chunks_of(zn):
    return CHUNKS if zn == 16 else tuple((d,) for d in range(zn))


def order_of(count):
    return [int(c) for c in ORDER] if count == 8 else [c for c in range(count) for _ in range(7)]


def kernel(
    zn,
    tokens_hbm,
    gain,
    ids,
    gates,
    w_gate,
    w_up,
    w_down,
    out,
    tokens,
    t_sem,
    sbuf,
    xb,
    fb,
    xr,
    hb,
    wgv,
    wuv,
    wdv,
    pf,
    pb,
    rsb,
    gb,
    rb,
    ret,
    vb,
    wl_sem,
    ws_sem,
    wr_sem,
    ds_sem,
    dr_sem,
    ys_sem,
    yr_sem,
    xs_sem,
    xr_sem,
    hs_sem,
    hr_sem,
    rs_sem,
    rr_sem,
    os_sem,
    or_sem,
):
    zc, xc, cc, yc = (lax.axis_index(a) for a in ("z", "x", "core", "tp"))
    chunks = chunks_of(zn)
    offsets = [d for chunk in chunks for d in chunk]
    messages = 2 * len(offsets)
    starts = [0]
    for chunk in chunks:
        starts.append(starts[-1] + 2 * len(chunk))
    row_count, width = tokens_hbm.shape
    pieces = width // 128
    units = w_gate.shape[1]
    out_pieces = w_down.shape[1] // 128

    other_x = XN - 1 - xc
    pair_x = xc + 1 - 2 * lax.rem(xc, 2)
    up_y, down_y = lax.rem(yc + 1, YN), lax.rem(yc + YN - 1, YN)
    sibling = (zc, xc, 1 - cc, yc)
    pair = (zc, pair_x, cc, yc)
    sides = ((zc, xc, cc, up_y), (zc, xc, cc, down_y))

    def far(m, sign):
        d = offsets[m // 2] * sign
        return (lax.rem(zc + d + zn, zn), xc if m % 2 == 0 else other_x, 1 - cc, yc)

    token_copy = pltpu.make_async_copy(tokens_hbm, tokens, t_sem)
    token_copy.start()
    barrier = pltpu.get_barrier_semaphore()
    greeted = [far(m, 1) for m in range(messages)] + [pair, *sides]
    for device in greeted:
        pl.semaphore_signal(barrier, inc=1, device_id=device, device_id_type=MESH)

    weights = ((w_gate, wgv), (w_up, wuv), (w_down, wdv))
    own_weights = [pltpu.make_async_copy(src, dst.at[0], wl_sem.at[i]) for i, (src, dst) in enumerate(weights)]
    for copy in own_weights:
        copy.start()

    token_copy.wait()
    wide = tokens[...].astype(F32)
    scale = lax.rsqrt(jnp.mean(wide * wide, axis=-1, keepdims=True) + EPS)
    normed = (wide * scale * gain[...]).astype(BF16)

    earlier = (
        lax.broadcasted_iota(jnp.int32, (row_count, row_count), 0)
        < lax.broadcasted_iota(jnp.int32, (row_count, row_count), 1)
    )
    earlier = jnp.where(earlier, 1.0, 0.0).astype(BF16)
    first_id, second_id = ids[0:1, :], ids[1:2, :]

    def expert_of(message):
        expert = jnp.zeros_like(message) - 1
        for m in range(messages):
            z, x, _, _ = far(m, 1)
            expert = jnp.where(message == m, z * (XN // 2) + x // 2, expert)
        return expert

    def selection(message, slot):
        expert = expert_of(message)
        hit_first, hit_second = first_id == expert, second_id == expert
        hit = jnp.where(hit_first | hit_second, 1.0, 0.0)
        rank = jnp.dot(hit.astype(BF16), earlier, preferred_element_type=F32)
        taken = jnp.where(rank == slot.astype(F32), hit, 0.0)
        return taken, hit_first

    line = lax.broadcasted_iota(jnp.int32, (128, 1), 0)
    taken, _ = selection(line // K3, K3 * yc + line % K3)
    sent_rows = messages * K3
    placed = jnp.dot(taken.astype(BF16), normed, preferred_element_type=F32)
    for i in range(pieces):
        fb[pl.ds(i, sent_rows, stride=pieces), :] = placed[:sent_rows, i * 128 : (i + 1) * 128]
    sbuf[...] = fb[0 : sent_rows * pieces, :].reshape(sent_rows, pieces, 128).astype(BF16)

    pl.semaphore_wait(barrier, len(greeted))

    sends = []

    def remote(src, dst, send_sem, recv_sem, device, later=True):
        copy = pltpu.make_async_remote_copy(
            src_ref=src, dst_ref=dst, send_sem=send_sem, recv_sem=recv_sem, device_id=device, device_id_type=MESH
        )
        copy.start()
        if later:
            sends.append(copy)
        return copy

    def arrived(ref, sem):
        pltpu.make_async_copy(ref, ref, sem).wait()

    for c in range(len(chunks)):
        for m in range(starts[c], starts[c + 1]):
            rows = pl.ds(m * K3, K3)
            remote(sbuf.at[rows], xb.at[0, yc, rows], ds_sem.at[c], dr_sem.at[c], far(m, 1), later=False)
    shared_weights = [
        remote(src, dst.at[1], ws_sem.at[i], wr_sem.at[i], sibling) for i, (src, dst) in enumerate(weights)
    ]

    line = lax.broadcasted_iota(jnp.int32, (messages * CAP, 1), 0)
    taken, hit_first = selection(line // CAP, line % CAP)
    mix = jnp.transpose(taken * jnp.where(hit_first, gates[0:1, :], gates[1:2, :]))

    def run(c):
        m0, m1 = starts[c], starts[c + 1]
        return pl.ds(m0 * K3, (m1 - m0) * K3)

    def half(c, side):
        m0, m1 = starts[c], starts[c + 1]
        count = (m1 - m0) // 2 * K3
        return pl.ds(m0 * K3 + side * count, count)

    origin = [lax.rem(yc - r + YN, YN) for r in range(YN)]
    handles = {}

    def own_rows(c):
        block = xb.at[0, yc, run(c)]
        arrived(block, dr_sem.at[c])
        for side in (0, 1):
            handles["y", c, side] = remote(
                block, block, ys_sem.at[c, side], yr_sem.at[c, side], sides[side]
            )
        handles["x", c, 0] = remote(block, xb.at[1, yc, run(c)], xs_sem.at[c, 0], xr_sem.at[c, 0], pair)

    def next_rows(c):
        for side in (0, 1):
            handles["y", c, side].wait_recv()
            rel = 1 + 2 * side
            part = xb.at[0, origin[rel], half(c, side)]
            handles["f", c, side] = remote(
                part,
                part,
                ys_sem.at[c, 2 + side],
                yr_sem.at[c, 2 + side],
                sides[side],
            )
            handles["x", c, rel] = remote(
                xb.at[0, origin[rel], run(c)],
                xb.at[1, origin[rel], run(c)],
                xs_sem.at[c, rel],
                xr_sem.at[c, rel],
                pair,
            )

    def last_rows(c):
        for side in (0, 1):
            handles["f", c, side].wait_recv()
        handles["x", c, 2] = remote(
            xb.at[0, origin[2], run(c)], xb.at[1, origin[2], run(c)], xs_sem.at[c, 2], xr_sem.at[c, 2], pair
        )

    def chunk_rows(c):
        count = 2 * CAP * (starts[c + 1] - starts[c])
        return 2 * CAP * starts[c], count

    def first_product(c):
        for rel in range(YN):
            handles["x", c, rel].wait_recv()
        if not handles.get("weights"):
            handles["weights"] = True
            for copy in own_weights:
                copy.wait()
            for copy in shared_weights:
                copy.wait_recv()
        r0, count = chunk_rows(c)
        m0, m1 = starts[c], starts[c + 1]
        for side in (0, 1):
            for m in range(m0, m1):
                for y in range(YN):
                    at = ((side * (m1 - m0) + m - m0) * CAP + y * K3) * pieces
                    block = xb[side, y, m * K3 : (m + 1) * K3].astype(F32)
                    fb[at : at + K3 * pieces, :] = block.reshape(K3 * pieces, 128)
        for i in range(pieces):
            xr[0:count, i * 128 : (i + 1) * 128] = fb[pl.ds(i, count, stride=pieces), :].astype(BF16)
        for core in range(CN):
            gate = jnp.dot(xr[0:count, :], wgv[core], preferred_element_type=F32)
            upper = jnp.dot(xr[0:count, :], wuv[core], preferred_element_type=F32)
            hidden = gate / (1.0 + jnp.exp(-gate)) * upper
            hb[0, r0 : r0 + count, core * units : (core + 1) * units] = hidden.astype(BF16)
        for side in (0, 1):
            handles["h", c, side] = remote(
                hb.at[0, pl.ds(r0, count)],
                hb.at[1 + 2 * side, pl.ds(r0, count)],
                hs_sem.at[c, side],
                hr_sem.at[c, side],
                sides[side],
            )

    def next_hidden(c):
        r0, count = chunk_rows(c)
        for side in (0, 1):
            handles["h", c, side].wait_recv()
            rows = pl.ds(r0 + side * (count // 2), count // 2)
            handles["k", c, side] = remote(
                hb.at[1 + 2 * side, rows],
                hb.at[2, rows],
                hs_sem.at[c, 2 + side],
                hr_sem.at[c, 2 + side],
                sides[side],
            )

    def second_product(c):
        for side in (0, 1):
            handles["k", c, side].wait_recv()
        r0, count = chunk_rows(c)
        total = None
        for rel in range(YN):
            first = pl.multiple_of(origin[rel] * units, units)
            for core in range(CN):
                term = jnp.dot(
                    hb[rel, r0 : r0 + count, core * units : (core + 1) * units],
                    wdv[core, pl.ds(first, units), :],
                    preferred_element_type=F32,
                )
                total = term if total is None else total + term
        at, part = r0 // 2, count // 2
        pf[at : at + part, :] = total[0:part]
        pb[at : at + part, :] = total[part:count].astype(BF16)
        handles["r", c] = remote(
            pb.at[pl.ds(at, part)], rsb.at[pl.ds(at, part)], rs_sem.at[c], rr_sem.at[c], pair
        )

    def give_back(c):
        handles["r", c].wait_recv()
        r0, count = chunk_rows(c)
        at, part = r0 // 2, count // 2
        total = pf[at : at + part, :] + rsb[at : at + part, :].astype(F32)
        for i in range(out_pieces):
            gb[pl.ds(i, part, stride=out_pieces), :] = total[:, i * 128 : (i + 1) * 128]
        rb[at * out_pieces : (at + part) * out_pieces, :] = gb[0 : part * out_pieces, :].astype(BF16)
        size = CAP * out_pieces
        for m in range(starts[c], starts[c + 1]):
            rows = pl.ds(m * size, size)
            remote(rb.at[rows], ret.at[rows], os_sem.at[c], or_sem.at[c], far(m, -1), later=False)

    stages = (own_rows, next_rows, last_rows, first_product, next_hidden, second_product, give_back)
    reached = [0] * len(chunks)
    for c in order_of(len(chunks)):
        stages[reached[c]](c)
        reached[c] += 1

    size = CAP * out_pieces
    for c in range(len(chunks)):
        m0, m1 = starts[c], starts[c + 1]
        arrived(ret.at[pl.ds(m0 * size, (m1 - m0) * size)], or_sem.at[c])
    gb[0 : messages * size, :] = ret[...].astype(F32)
    for i in range(out_pieces):
        vb[:, i * 128 : (i + 1) * 128] = gb[pl.ds(i, messages * CAP, stride=out_pieces), :].astype(BF16)
    values = vb[...]
    high = mix.astype(BF16)
    rest = mix - high.astype(F32)
    middle = rest.astype(BF16)
    low = (rest - middle.astype(F32)).astype(BF16)
    mixed = jnp.dot(high, values, preferred_element_type=F32)
    mixed = mixed + jnp.dot(middle, values, preferred_element_type=F32)
    mixed = mixed + jnp.dot(low, values, preferred_element_type=F32)
    out[...] = mixed.astype(BF16)

    for copy in sends:
        copy.wait_send()
    for c in range(len(chunks)):
        m0, m1 = starts[c], starts[c + 1]
        arrived(sbuf.at[pl.ds(m0 * K3, (m1 - m0) * K3)], ds_sem.at[c])
        arrived(rb.at[pl.ds(m0 * size, (m1 - m0) * size)], os_sem.at[c])


def on_device(zn, tokens, norm_gain, expert_ids, gate_weights, w_gate, w_up, w_down):
    chunks = chunks_of(zn)
    n = len(chunks)
    messages = 2 * sum(len(chunk) for chunk in chunks)
    most = 2 * max(len(chunk) for chunk in chunks)
    row_count, width = tokens.shape
    pieces = width // 128
    units = w_gate.shape[1]
    block, columns = w_down.shape
    out_pieces = columns // 128
    rows = messages * CAP
    dma = pltpu.SemaphoreType.DMA
    scratch = [
        pltpu.VMEM((row_count, width), BF16),
        dma(()),
        pltpu.VMEM((messages * K3, pieces, 128), BF16),
        pltpu.VMEM((2, YN, messages * K3, pieces, 128), BF16),
        pltpu.VMEM((max(2 * most * CAP, messages * K3) * pieces, 128), F32),
        pltpu.VMEM((2 * most * CAP, width), BF16),
        pltpu.VMEM((YN, 2 * rows, CN * units), BF16),
        pltpu.VMEM((CN, width, units), BF16),
        pltpu.VMEM((CN, width, units), BF16),
        pltpu.VMEM((CN, block, columns), BF16),
        pltpu.VMEM((rows, columns), F32),
        pltpu.VMEM((rows, columns), BF16),
        pltpu.VMEM((rows, columns), BF16),
        pltpu.VMEM((rows * out_pieces, 128), F32),
        pltpu.VMEM((rows * out_pieces, 128), BF16),
        pltpu.VMEM((rows * out_pieces, 128), BF16),
        pltpu.VMEM((rows, columns), BF16),
        dma((3,)),
        dma((3,)),
        dma((3,)),
        dma((n,)),
        dma((n,)),
        dma((n, 4)),
        dma((n, 4)),
        dma((n, 4)),
        dma((n, 4)),
        dma((n, 4)),
        dma((n, 4)),
        dma((n,)),
        dma((n,)),
        dma((n,)),
        dma((n,)),
    ]
    vmem = pl.BlockSpec(memory_space=pltpu.VMEM)
    hbm = pl.BlockSpec(memory_space=pl.ANY)
    return pl.pallas_call(
        functools.partial(kernel, zn),
        out_shape=jax.ShapeDtypeStruct((row_count, columns), BF16),
        in_specs=[hbm, vmem, vmem, vmem, hbm, hbm, hbm],
        out_specs=vmem,
        scratch_shapes=scratch,
        compiler_params=pltpu.CompilerParams(
            collective_id=0, has_side_effects=True, vmem_limit_bytes=60 * 1024 * 1024
        ),
        name="expert_layer",
    )(tokens, norm_gain.reshape(1, width), expert_ids.T, gate_weights.T, w_gate, w_up, w_down)


def solution(mesh):
    zn = mesh.shape["ep"] // (XN * CN)
    finer = Mesh(mesh.devices.reshape(zn, XN, CN, mesh.shape["tp"]), (*EP, "tp"))
    placed = (
        P(EP, None),
        P(),
        P(EP, None),
        P(EP, None),
        P(None, (*EP, "tp")),
        P(None, (*EP, "tp")),
        P(EP, "tp"),
    )
    return jax.shard_map(
        functools.partial(on_device, zn), mesh=finer, in_specs=placed, out_specs=P(EP, "tp"), check_vma=False
    )
```

```python
import functools

import jax
import jax.numpy as jnp
from jax import lax
from jax.experimental import pallas as pl
from jax.experimental.pallas import tpu as pltpu
from jax.sharding import Mesh
from jax.sharding import PartitionSpec as P

MESH = pl.DeviceIdType.MESH
EP = ("z", "x", "core")
EPS = 1e-06
XN = 4
CN = 2
YN = 4
K3 = 3
CAP = YN * K3
CHUNKS = ((2, -2), (4, -4), (8, 0), (1, -1), (7, -7), (-6, 6), (-5, 5), (-3, 3))
ORDER = "01030121402451462057145062146752401735643275632756376373"

BF16 = jnp.bfloat16
F32 = jnp.float32


def chunks_of(zn):
    return CHUNKS if zn == 16 else tuple((d,) for d in range(zn))


def order_of(count):
    return [int(c) for c in ORDER] if count == 8 else [c for c in range(count) for _ in range(7)]


def kernel(
    zn,
    tokens_hbm,
    gain,
    ids,
    gates,
    w_gate,
    w_up,
    w_down,
    out,
    tokens,
    t_sem,
    sbuf,
    xb,
    fb,
    xr,
    hb,
    wgv,
    wuv,
    wdv,
    pf,
    pb,
    rsb,
    gb,
    rb,
    ret,
    vb,
    wl_sem,
    ws_sem,
    wr_sem,
    ds_sem,
    dr_sem,
    ys_sem,
    yr_sem,
    xs_sem,
    xr_sem,
    hs_sem,
    hr_sem,
    rs_sem,
    rr_sem,
    os_sem,
    or_sem,
):
    zc, xc, cc, yc = (lax.axis_index(a) for a in ("z", "x", "core", "tp"))
    chunks = chunks_of(zn)
    offsets = [d for chunk in chunks for d in chunk]
    messages = 2 * len(offsets)
    starts = [0]
    for chunk in chunks:
        starts.append(starts[-1] + 2 * len(chunk))
    row_count, width = tokens_hbm.shape
    pieces = width // 128
    units = w_gate.shape[1]
    out_pieces = w_down.shape[1] // 128

    other_x = XN - 1 - xc
    pair_x = xc + 1 - 2 * lax.rem(xc, 2)
    up_y, down_y = lax.rem(yc + 1, YN), lax.rem(yc + YN - 1, YN)
    sibling = (zc, xc, 1 - cc, yc)
    pair = (zc, pair_x, cc, yc)
    sides = ((zc, xc, cc, up_y), (zc, xc, cc, down_y))

    def far(m, sign):
        d = offsets[m // 2] * sign
        return (lax.rem(zc + d + zn, zn), xc if m % 2 == 0 else other_x, 1 - cc, yc)

    token_copy = pltpu.make_async_copy(tokens_hbm, tokens, t_sem)
    token_copy.start()
    barrier = pltpu.get_barrier_semaphore()
    greeted = [far(m, 1) for m in range(messages)] + [pair, *sides]
    for device in greeted:
        pl.semaphore_signal(barrier, inc=1, device_id=device, device_id_type=MESH)

    weights = ((w_gate, wgv), (w_up, wuv), (w_down, wdv))
    own_weights = [pltpu.make_async_copy(src, dst.at[0], wl_sem.at[i]) for i, (src, dst) in enumerate(weights)]
    for copy in own_weights:
        copy.start()

    token_copy.wait()
    wide = tokens[...].astype(F32)
    scale = lax.rsqrt(jnp.mean(wide * wide, axis=-1, keepdims=True) + EPS)
    normed = (wide * scale * gain[...]).astype(BF16)

    earlier = (
        lax.broadcasted_iota(jnp.int32, (row_count, row_count), 0)
        < lax.broadcasted_iota(jnp.int32, (row_count, row_count), 1)
    )
    earlier = jnp.where(earlier, 1.0, 0.0).astype(BF16)
    first_id, second_id = ids[0:1, :], ids[1:2, :]

    def expert_of(message):
        expert = jnp.zeros_like(message) - 1
        for m in range(messages):
            z, x, _, _ = far(m, 1)
            expert = jnp.where(message == m, z * (XN // 2) + x // 2, expert)
        return expert

    def selection(message, slot):
        expert = expert_of(message)
        hit_first, hit_second = first_id == expert, second_id == expert
        hit = jnp.where(hit_first | hit_second, 1.0, 0.0)
        rank = jnp.dot(hit.astype(BF16), earlier, preferred_element_type=F32)
        taken = jnp.where(rank == slot.astype(F32), hit, 0.0)
        return taken, hit_first

    line = lax.broadcasted_iota(jnp.int32, (128, 1), 0)
    taken, _ = selection(line // K3, K3 * yc + line % K3)
    sent_rows = messages * K3
    placed = jnp.dot(taken.astype(BF16), normed, preferred_element_type=F32)
    for i in range(pieces):
        fb[pl.ds(i, sent_rows, stride=pieces), :] = placed[:sent_rows, i * 128 : (i + 1) * 128]
    sbuf[...] = fb[0 : sent_rows * pieces, :].reshape(sent_rows, pieces, 128).astype(BF16)

    pl.semaphore_wait(barrier, len(greeted))

    def remote(src, dst, send_sem, recv_sem, device):
        copy = pltpu.make_async_remote_copy(
            src_ref=src, dst_ref=dst, send_sem=send_sem, recv_sem=recv_sem, device_id=device, device_id_type=MESH
        )
        copy.start()
        return copy

    def arrived(ref, sem):
        pltpu.make_async_copy(ref, ref, sem).wait()

    for c in range(len(chunks)):
        for m in range(starts[c], starts[c + 1]):
            rows = pl.ds(m * K3, K3)
            remote(sbuf.at[rows], xb.at[0, yc, rows], ds_sem, dr_sem.at[c], far(m, 1))
    shared_weights = [
        remote(src, dst.at[1], ws_sem.at[i], wr_sem.at[i], sibling) for i, (src, dst) in enumerate(weights)
    ]

    line = lax.broadcasted_iota(jnp.int32, (messages * CAP, 1), 0)
    taken, hit_first = selection(line // CAP, line % CAP)
    mix = jnp.transpose(taken * jnp.where(hit_first, gates[0:1, :], gates[1:2, :]))

    def run(c):
        m0, m1 = starts[c], starts[c + 1]
        return pl.ds(m0 * K3, (m1 - m0) * K3)

    def half(c, side):
        m0, m1 = starts[c], starts[c + 1]
        count = (m1 - m0) // 2 * K3
        return pl.ds(m0 * K3 + side * count, count)

    origin = [lax.rem(yc - r + YN, YN) for r in range(YN)]
    handles = {}

    def own_rows(c):
        block = xb.at[0, yc, run(c)]
        arrived(block, dr_sem.at[c])
        for side in (0, 1):
            handles["y", c, side] = remote(
                block, block, ys_sem, yr_sem.at[c, side], sides[side]
            )
        handles["x", c, 0] = remote(block, xb.at[1, yc, run(c)], xs_sem, xr_sem.at[c], pair)

    def next_rows(c):
        for side in (0, 1):
            handles["y", c, side].wait_recv()
            rel = 1 + 2 * side
            part = xb.at[0, origin[rel], half(c, side)]
            handles["f", c, side] = remote(
                part,
                part,
                ys_sem,
                yr_sem.at[c, 2],
                sides[side],
            )
            handles["x", c, rel] = remote(
                xb.at[0, origin[rel], run(c)],
                xb.at[1, origin[rel], run(c)],
                xs_sem,
                xr_sem.at[c],
                pair,
            )

    def last_rows(c):
        arrived(xb.at[0, origin[2], run(c)], yr_sem.at[c, 2])
        handles["x", c, 2] = remote(
            xb.at[0, origin[2], run(c)], xb.at[1, origin[2], run(c)], xs_sem, xr_sem.at[c], pair
        )

    def chunk_rows(c):
        count = 2 * CAP * (starts[c + 1] - starts[c])
        return 2 * CAP * starts[c], count

    def first_product(c):
        arrived(xb.at[1, :, run(c)], xr_sem.at[c])
        if not handles.get("weights"):
            handles["weights"] = True
            for copy in own_weights:
                copy.wait()
            for copy in shared_weights:
                copy.wait_recv()
        r0, count = chunk_rows(c)
        m0, m1 = starts[c], starts[c + 1]
        for side in (0, 1):
            for m in range(m0, m1):
                for y in range(YN):
                    at = ((side * (m1 - m0) + m - m0) * CAP + y * K3) * pieces
                    block = xb[side, y, m * K3 : (m + 1) * K3].astype(F32)
                    fb[at : at + K3 * pieces, :] = block.reshape(K3 * pieces, 128)
        for i in range(pieces):
            xr[0:count, i * 128 : (i + 1) * 128] = fb[pl.ds(i, count, stride=pieces), :].astype(BF16)
        for core in range(CN):
            gate = jnp.dot(xr[0:count, :], wgv[core], preferred_element_type=F32)
            upper = jnp.dot(xr[0:count, :], wuv[core], preferred_element_type=F32)
            hidden = gate / (1.0 + jnp.exp(-gate)) * upper
            hb[0, r0 : r0 + count, core * units : (core + 1) * units] = hidden.astype(BF16)
        for side in (0, 1):
            handles["h", c, side] = remote(
                hb.at[0, pl.ds(r0, count)],
                hb.at[1 + 2 * side, pl.ds(r0, count)],
                hs_sem,
                hr_sem.at[c, side],
                sides[side],
            )

    def next_hidden(c):
        r0, count = chunk_rows(c)
        for side in (0, 1):
            handles["h", c, side].wait_recv()
            rows = pl.ds(r0 + side * (count // 2), count // 2)
            handles["k", c, side] = remote(
                hb.at[1 + 2 * side, rows],
                hb.at[2, rows],
                hs_sem,
                hr_sem.at[c, 2],
                sides[side],
            )

    def second_product(c):
        r0, count = chunk_rows(c)
        arrived(hb.at[2, pl.ds(r0, count)], hr_sem.at[c, 2])
        total = None
        for rel in range(YN):
            first = pl.multiple_of(origin[rel] * units, units)
            for core in range(CN):
                term = jnp.dot(
                    hb[rel, r0 : r0 + count, core * units : (core + 1) * units],
                    wdv[core, pl.ds(first, units), :],
                    preferred_element_type=F32,
                )
                total = term if total is None else total + term
        at, part = r0 // 2, count // 2
        pf[at : at + part, :] = total[0:part]
        pb[at : at + part, :] = total[part:count].astype(BF16)
        handles["r", c] = remote(
            pb.at[pl.ds(at, part)], rsb.at[pl.ds(at, part)], rs_sem, rr_sem.at[c], pair
        )

    def give_back(c):
        handles["r", c].wait_recv()
        r0, count = chunk_rows(c)
        at, part = r0 // 2, count // 2
        total = pf[at : at + part, :] + rsb[at : at + part, :].astype(F32)
        for i in range(out_pieces):
            gb[pl.ds(i, part, stride=out_pieces), :] = total[:, i * 128 : (i + 1) * 128]
        rb[at * out_pieces : (at + part) * out_pieces, :] = gb[0 : part * out_pieces, :].astype(BF16)
        size = CAP * out_pieces
        for m in range(starts[c], starts[c + 1]):
            rows = pl.ds(m * size, size)
            remote(rb.at[rows], ret.at[rows], os_sem, or_sem, far(m, -1))

    stages = (own_rows, next_rows, last_rows, first_product, next_hidden, second_product, give_back)
    reached = [0] * len(chunks)
    for c in order_of(len(chunks)):
        stages[reached[c]](c)
        reached[c] += 1

    size = CAP * out_pieces
    arrived(ret, or_sem)
    gb[0 : messages * size, :] = ret[...].astype(F32)
    for i in range(out_pieces):
        vb[:, i * 128 : (i + 1) * 128] = gb[pl.ds(i, messages * CAP, stride=out_pieces), :].astype(BF16)
    values = vb[...]
    high = mix.astype(BF16)
    rest = mix - high.astype(F32)
    middle = rest.astype(BF16)
    low = (rest - middle.astype(F32)).astype(BF16)
    mixed = jnp.dot(high, values, preferred_element_type=F32)
    mixed = mixed + jnp.dot(middle, values, preferred_element_type=F32)
    mixed = mixed + jnp.dot(low, values, preferred_element_type=F32)
    out[...] = mixed.astype(BF16)

    for copy in shared_weights:
        copy.wait_send()
    three = pl.ds(0, YN - 1)
    for ref, sem in (
        (sbuf, ds_sem),
        (xb.at[0, three], ys_sem),
        (xb.at[1], xs_sem),
        (hb.at[three], hs_sem),
        (pb, rs_sem),
        (rb, os_sem),
    ):
        arrived(ref, sem)


def on_device(zn, tokens, norm_gain, expert_ids, gate_weights, w_gate, w_up, w_down):
    chunks = chunks_of(zn)
    n = len(chunks)
    messages = 2 * sum(len(chunk) for chunk in chunks)
    most = 2 * max(len(chunk) for chunk in chunks)
    row_count, width = tokens.shape
    pieces = width // 128
    units = w_gate.shape[1]
    block, columns = w_down.shape
    out_pieces = columns // 128
    rows = messages * CAP
    dma = pltpu.SemaphoreType.DMA
    scratch = [
        pltpu.VMEM((row_count, width), BF16),
        dma(()),
        pltpu.VMEM((messages * K3, pieces, 128), BF16),
        pltpu.VMEM((2, YN, messages * K3, pieces, 128), BF16),
        pltpu.VMEM((max(2 * most * CAP, messages * K3) * pieces, 128), F32),
        pltpu.VMEM((2 * most * CAP, width), BF16),
        pltpu.VMEM((YN, 2 * rows, CN * units), BF16),
        pltpu.VMEM((CN, width, units), BF16),
        pltpu.VMEM((CN, width, units), BF16),
        pltpu.VMEM((CN, block, columns), BF16),
        pltpu.VMEM((rows, columns), F32),
        pltpu.VMEM((rows, columns), BF16),
        pltpu.VMEM((rows, columns), BF16),
        pltpu.VMEM((rows * out_pieces, 128), F32),
        pltpu.VMEM((rows * out_pieces, 128), BF16),
        pltpu.VMEM((rows * out_pieces, 128), BF16),
        pltpu.VMEM((rows, columns), BF16),
        dma((3,)),
        dma((3,)),
        dma((3,)),
        dma(()),
        dma((n,)),
        dma(()),
        dma((n, 3)),
        dma(()),
        dma((n,)),
        dma(()),
        dma((n, 3)),
        dma(()),
        dma((n,)),
        dma(()),
        dma(()),
    ]
    vmem = pl.BlockSpec(memory_space=pltpu.VMEM)
    hbm = pl.BlockSpec(memory_space=pl.ANY)
    return pl.pallas_call(
        functools.partial(kernel, zn),
        out_shape=jax.ShapeDtypeStruct((row_count, columns), BF16),
        in_specs=[hbm, vmem, vmem, vmem, hbm, hbm, hbm],
        out_specs=vmem,
        scratch_shapes=scratch,
        compiler_params=pltpu.CompilerParams(
            collective_id=0, has_side_effects=True, vmem_limit_bytes=60 * 1024 * 1024
        ),
        name="expert_layer",
    )(tokens, norm_gain.reshape(1, width), expert_ids.T, gate_weights.T, w_gate, w_up, w_down)


def solution(mesh):
    zn = mesh.shape["ep"] // (XN * CN)
    finer = Mesh(mesh.devices.reshape(zn, XN, CN, mesh.shape["tp"]), (*EP, "tp"))
    placed = (
        P(EP, None),
        P(),
        P(EP, None),
        P(EP, None),
        P(None, (*EP, "tp")),
        P(None, (*EP, "tp")),
        P(EP, "tp"),
    )
    return jax.shard_map(
        functools.partial(on_device, zn), mesh=finer, in_specs=placed, out_specs=P(EP, "tp"), check_vma=False
    )
```

```python
import functools

import jax
import jax.numpy as jnp
from jax import lax
from jax.experimental import pallas as pl
from jax.experimental.pallas import tpu as pltpu
from jax.sharding import Mesh
from jax.sharding import PartitionSpec as P

MESH = pl.DeviceIdType.MESH
EP = ("z", "x", "core")
EPS = 1e-06
XN = 4
CN = 2
YN = 4
K3 = 3
CAP = YN * K3
CHUNKS = ((2, -2), (-5, 5), (7, -7), (4, -4), (8, 0), (1, -1), (-6, 6), (-3, 3))
ORDER = "00101213024312467124630254617325741603524670354673567575"

BF16 = jnp.bfloat16
F32 = jnp.float32


def chunks_of(zn):
    return CHUNKS if zn == 16 else tuple((d,) for d in range(zn))


def order_of(count):
    return [int(c) for c in ORDER] if count == 8 else [c for c in range(count) for _ in range(7)]


def kernel(
    zn,
    tokens_hbm,
    gain_hbm,
    ids_hbm,
    gates_hbm,
    w_gate,
    w_up,
    w_down,
    out,
    tokens,
    gain,
    ids,
    gates,
    t_sem,
    sbuf,
    xb,
    fb,
    xr,
    hb,
    wgv,
    wuv,
    wdv,
    pf,
    pb,
    rsb,
    gb,
    rb,
    ret,
    vb,
    wl_sem,
    ws_sem,
    wr_sem,
    ds_sem,
    dr_sem,
    ys_sem,
    yr_sem,
    xs_sem,
    xr_sem,
    hs_sem,
    hr_sem,
    rs_sem,
    rr_sem,
    os_sem,
    or_sem,
):
    zc, xc, cc, yc = (lax.axis_index(a) for a in ("z", "x", "core", "tp"))
    chunks = chunks_of(zn)
    offsets = [d for chunk in chunks for d in chunk]
    messages = 2 * len(offsets)
    starts = [0]
    for chunk in chunks:
        starts.append(starts[-1] + 2 * len(chunk))
    row_count, width = tokens_hbm.shape
    pieces = width // 128
    units = w_gate.shape[1]
    out_pieces = w_down.shape[1] // 128

    other_x = XN - 1 - xc
    pair_x = xc + 1 - 2 * lax.rem(xc, 2)
    up_y, down_y = lax.rem(yc + 1, YN), lax.rem(yc + YN - 1, YN)
    sibling = (zc, xc, 1 - cc, yc)
    pair = (zc, pair_x, cc, yc)
    sides = ((zc, xc, cc, up_y), (zc, xc, cc, down_y))

    def far(m, sign):
        d = offsets[m // 2] * sign
        return (lax.rem(zc + d + zn, zn), xc if m % 2 == 0 else other_x, 1 - cc, yc)

    small = ((tokens_hbm, tokens), (gain_hbm, gain), (ids_hbm, ids), (gates_hbm, gates))
    inputs = [pltpu.make_async_copy(src, dst, t_sem.at[i]) for i, (src, dst) in enumerate(small)]
    for copy in inputs:
        copy.start()
    barrier = pltpu.get_barrier_semaphore()
    greeted = [far(m, 1) for m in range(messages)] + [pair, *sides]
    for device in greeted:
        pl.semaphore_signal(barrier, inc=1, device_id=device, device_id_type=MESH)

    weights = ((w_gate, wgv), (w_up, wuv), (w_down, wdv))
    own_weights = [pltpu.make_async_copy(src, dst.at[0], wl_sem.at[i]) for i, (src, dst) in enumerate(weights)]
    for copy in own_weights:
        copy.start()

    for copy in inputs:
        copy.wait()
    wide = tokens[...].astype(F32)
    scale = lax.rsqrt(jnp.mean(wide * wide, axis=-1, keepdims=True) + EPS)
    normed = (wide * scale * gain[...]).astype(BF16)

    earlier = (
        lax.broadcasted_iota(jnp.int32, (row_count, row_count), 0)
        < lax.broadcasted_iota(jnp.int32, (row_count, row_count), 1)
    )
    earlier = jnp.where(earlier, 1.0, 0.0).astype(BF16)
    first_id, second_id = ids[0:1, :], ids[1:2, :]

    def expert_of(message):
        expert = jnp.zeros_like(message) - 1
        for m in range(messages):
            z, x, _, _ = far(m, 1)
            expert = jnp.where(message == m, z * (XN // 2) + x // 2, expert)
        return expert

    def selection(message, slot):
        expert = expert_of(message)
        hit_first, hit_second = first_id == expert, second_id == expert
        hit = jnp.where(hit_first | hit_second, 1.0, 0.0)
        rank = jnp.dot(hit.astype(BF16), earlier, preferred_element_type=F32)
        taken = jnp.where(rank == slot.astype(F32), hit, 0.0)
        return taken, hit_first

    line = lax.broadcasted_iota(jnp.int32, (128, 1), 0)
    taken, _ = selection(line // K3, K3 * yc + line % K3)
    sent_rows = messages * K3
    placed = jnp.dot(taken.astype(BF16), normed, preferred_element_type=F32)
    for i in range(pieces):
        fb[pl.ds(i, sent_rows, stride=pieces), :] = placed[:sent_rows, i * 128 : (i + 1) * 128]
    sbuf[...] = fb[0 : sent_rows * pieces, :].reshape(sent_rows, pieces, 128).astype(BF16)

    pl.semaphore_wait(barrier, len(greeted))

    def remote(src, dst, send_sem, recv_sem, device):
        copy = pltpu.make_async_remote_copy(
            src_ref=src, dst_ref=dst, send_sem=send_sem, recv_sem=recv_sem, device_id=device, device_id_type=MESH
        )
        copy.start()
        return copy

    def arrived(ref, sem):
        pltpu.make_async_copy(ref, ref, sem).wait()

    for c in range(len(chunks)):
        for m in range(starts[c], starts[c + 1]):
            rows = pl.ds(m * K3, K3)
            remote(sbuf.at[rows], xb.at[0, yc, rows], ds_sem, dr_sem.at[c], far(m, 1))
    shared_weights = [
        remote(src, dst.at[1], ws_sem.at[i], wr_sem.at[i], sibling) for i, (src, dst) in enumerate(weights)
    ]

    line = lax.broadcasted_iota(jnp.int32, (messages * CAP, 1), 0)
    taken, hit_first = selection(line // CAP, line % CAP)
    mix = jnp.transpose(taken * jnp.where(hit_first, gates[0:1, :], gates[1:2, :]))

    def run(c):
        m0, m1 = starts[c], starts[c + 1]
        return pl.ds(m0 * K3, (m1 - m0) * K3)

    def half(c, side):
        m0, m1 = starts[c], starts[c + 1]
        count = (m1 - m0) // 2 * K3
        return pl.ds(m0 * K3 + side * count, count)

    origin = [lax.rem(yc - r + YN, YN) for r in range(YN)]
    handles = {}

    def own_rows(c):
        block = xb.at[0, yc, run(c)]
        arrived(block, dr_sem.at[c])
        for part in (0, 1):
            for side in (0, 1):
                rows = xb.at[0, yc, half(c, (side + part) % 2)]
                handles["y", c, side, part] = remote(rows, rows, ys_sem, yr_sem.at[c, 2 * part + side], sides[side])
        handles["x", c, 0] = remote(block, xb.at[1, yc, run(c)], xs_sem, xr_sem.at[c], pair)

    def next_rows(c):
        for side in (0, 1):
            rel = 1 + 2 * side
            part = xb.at[0, origin[rel], half(c, side)]
            arrived(part, yr_sem.at[c, side])
            remote(part, part, ys_sem, yr_sem.at[c, 4], sides[side])
        for side in (0, 1):
            rel = 1 + 2 * side
            arrived(xb.at[0, origin[rel], half(c, 1 - side)], yr_sem.at[c, 2 + side])
            handles["x", c, rel] = remote(
                xb.at[0, origin[rel], run(c)],
                xb.at[1, origin[rel], run(c)],
                xs_sem,
                xr_sem.at[c],
                pair,
            )

    def last_rows(c):
        arrived(xb.at[0, origin[2], run(c)], yr_sem.at[c, 4])
        handles["x", c, 2] = remote(
            xb.at[0, origin[2], run(c)], xb.at[1, origin[2], run(c)], xs_sem, xr_sem.at[c], pair
        )

    def chunk_rows(c):
        count = 2 * CAP * (starts[c + 1] - starts[c])
        return 2 * CAP * starts[c], count

    def first_product(c):
        arrived(xb.at[1, :, run(c)], xr_sem.at[c])
        if not handles.get("weights"):
            handles["weights"] = True
            for copy in own_weights:
                copy.wait()
            for copy in shared_weights:
                copy.wait_recv()
        r0, count = chunk_rows(c)
        m0, m1 = starts[c], starts[c + 1]
        for side in (0, 1):
            for m in range(m0, m1):
                for y in range(YN):
                    at = ((side * (m1 - m0) + m - m0) * CAP + y * K3) * pieces
                    block = xb[side, y, m * K3 : (m + 1) * K3].astype(F32)
                    fb[at : at + K3 * pieces, :] = block.reshape(K3 * pieces, 128)
        for i in range(pieces):
            xr[0:count, i * 128 : (i + 1) * 128] = fb[pl.ds(i, count, stride=pieces), :].astype(BF16)
        for core in range(CN):
            gate = jnp.dot(xr[0:count, :], wgv[core], preferred_element_type=F32)
            upper = jnp.dot(xr[0:count, :], wuv[core], preferred_element_type=F32)
            hidden = gate / (1.0 + jnp.exp(-gate)) * upper
            hb[0, core, r0 : r0 + count, :] = hidden.astype(BF16)
            give_hidden(c, core, core)
        for side in (0, 1):
            give_hidden(c, side, 1 - side)

    def hidden_rows(c, rel, core):
        r0, count = chunk_rows(c)
        return hb.at[rel, core, pl.ds(r0, count)]

    def give_hidden(c, side, core):
        sem = hr_sem.at[c, side if core == side else 2 + side]
        remote(hidden_rows(c, 0, core), hidden_rows(c, 1 + 2 * side, core), hs_sem, sem, sides[side])

    def next_hidden(c):
        for side in (0, 1):
            block = hidden_rows(c, 1 + 2 * side, side)
            arrived(block, hr_sem.at[c, side])
            remote(block, hidden_rows(c, 2, side), hs_sem, hr_sem.at[c, 4], sides[side])

    def second_product(c):
        r0, count = chunk_rows(c)
        for side in (0, 1):
            arrived(hidden_rows(c, 1 + 2 * side, 1 - side), hr_sem.at[c, 2 + side])
        arrived(hb.at[2, :, pl.ds(r0, count)], hr_sem.at[c, 4])
        total = None
        for rel in range(YN):
            first = pl.multiple_of(origin[rel] * units, units)
            for core in range(CN):
                term = jnp.dot(
                    hb[rel, core, r0 : r0 + count, :],
                    wdv[core, pl.ds(first, units), :],
                    preferred_element_type=F32,
                )
                total = term if total is None else total + term
        at, part = r0 // 2, count // 2
        pf[at : at + part, :] = total[0:part]
        pb[at : at + part, :] = total[part:count].astype(BF16)
        handles["r", c] = remote(
            pb.at[pl.ds(at, part)], rsb.at[pl.ds(at, part)], rs_sem, rr_sem.at[c], pair
        )

    def give_back(c):
        handles["r", c].wait_recv()
        r0, count = chunk_rows(c)
        at, part = r0 // 2, count // 2
        total = pf[at : at + part, :] + rsb[at : at + part, :].astype(F32)
        for i in range(out_pieces):
            gb[pl.ds(i, part, stride=out_pieces), :] = total[:, i * 128 : (i + 1) * 128]
        rb[at * out_pieces : (at + part) * out_pieces, :] = gb[0 : part * out_pieces, :].astype(BF16)
        size = CAP * out_pieces
        for m in range(starts[c], starts[c + 1]):
            rows = pl.ds(m * size, size)
            remote(rb.at[rows], ret.at[rows], os_sem, or_sem, far(m, -1))

    stages = (own_rows, next_rows, last_rows, first_product, next_hidden, second_product, give_back)
    reached = [0] * len(chunks)
    for c in order_of(len(chunks)):
        stages[reached[c]](c)
        reached[c] += 1

    size = CAP * out_pieces
    arrived(ret, or_sem)
    gb[0 : messages * size, :] = ret[...].astype(F32)
    for i in range(out_pieces):
        vb[:, i * 128 : (i + 1) * 128] = gb[pl.ds(i, messages * CAP, stride=out_pieces), :].astype(BF16)
    values = vb[...]
    high = mix.astype(BF16)
    rest = mix - high.astype(F32)
    middle = rest.astype(BF16)
    low = (rest - middle.astype(F32)).astype(BF16)
    mixed = jnp.dot(high, values, preferred_element_type=F32)
    mixed = mixed + jnp.dot(middle, values, preferred_element_type=F32)
    mixed = mixed + jnp.dot(low, values, preferred_element_type=F32)
    out[...] = mixed.astype(BF16)

    for copy in shared_weights:
        copy.wait_send()
    three = pl.ds(0, YN - 1)
    for ref, sem in (
        (sbuf, ds_sem),
        (xb.at[0, three], ys_sem),
        (xb.at[1], xs_sem),
        (hb.at[three], hs_sem),
        (pb, rs_sem),
        (rb, os_sem),
    ):
        arrived(ref, sem)


def on_device(zn, tokens, norm_gain, expert_ids, gate_weights, w_gate, w_up, w_down):
    chunks = chunks_of(zn)
    n = len(chunks)
    messages = 2 * sum(len(chunk) for chunk in chunks)
    most = 2 * max(len(chunk) for chunk in chunks)
    row_count, width = tokens.shape
    pieces = width // 128
    units = w_gate.shape[1]
    block, columns = w_down.shape
    out_pieces = columns // 128
    rows = messages * CAP
    dma = pltpu.SemaphoreType.DMA
    scratch = [
        pltpu.VMEM((row_count, width), BF16),
        pltpu.VMEM((1, width), F32),
        pltpu.VMEM((2, row_count), jnp.int32),
        pltpu.VMEM((2, row_count), F32),
        dma((4,)),
        pltpu.VMEM((messages * K3, pieces, 128), BF16),
        pltpu.VMEM((2, YN, messages * K3, pieces, 128), BF16),
        pltpu.VMEM((max(2 * most * CAP, messages * K3) * pieces, 128), F32),
        pltpu.VMEM((2 * most * CAP, width), BF16),
        pltpu.VMEM((YN, CN, 2 * rows, units), BF16),
        pltpu.VMEM((CN, width, units), BF16),
        pltpu.VMEM((CN, width, units), BF16),
        pltpu.VMEM((CN, block, columns), BF16),
        pltpu.VMEM((rows, columns), F32),
        pltpu.VMEM((rows, columns), BF16),
        pltpu.VMEM((rows, columns), BF16),
        pltpu.VMEM((rows * out_pieces, 128), F32),
        pltpu.VMEM((rows * out_pieces, 128), BF16),
        pltpu.VMEM((rows * out_pieces, 128), BF16),
        pltpu.VMEM((rows, columns), BF16),
        dma((3,)),
        dma((3,)),
        dma((3,)),
        dma(()),
        dma((n,)),
        dma(()),
        dma((n, 5)),
        dma(()),
        dma((n,)),
        dma(()),
        dma((n, 5)),
        dma(()),
        dma((n,)),
        dma(()),
        dma(()),
    ]
    vmem = pl.BlockSpec(memory_space=pltpu.VMEM)
    hbm = pl.BlockSpec(memory_space=pl.ANY)
    return pl.pallas_call(
        functools.partial(kernel, zn),
        out_shape=jax.ShapeDtypeStruct((row_count, columns), BF16),
        in_specs=[hbm] * 7,
        out_specs=vmem,
        scratch_shapes=scratch,
        compiler_params=pltpu.CompilerParams(
            collective_id=0, has_side_effects=True, vmem_limit_bytes=60 * 1024 * 1024
        ),
        name="expert_layer",
    )(tokens, norm_gain.reshape(1, width), expert_ids.T, gate_weights.T, w_gate, w_up, w_down)


def solution(mesh):
    zn = mesh.shape["ep"] // (XN * CN)
    finer = Mesh(mesh.devices.reshape(zn, XN, CN, mesh.shape["tp"]), (*EP, "tp"))
    placed = (
        P(EP, None),
        P(),
        P(EP, None),
        P(EP, None),
        P(None, (*EP, "tp")),
        P(None, (*EP, "tp")),
        P(EP, "tp"),
    )
    return jax.shard_map(
        functools.partial(on_device, zn), mesh=finer, in_specs=placed, out_specs=P(EP, "tp"), check_vma=False
    )
```

```python
import functools

import jax
import jax.numpy as jnp
from jax import lax
from jax.experimental import pallas as pl
from jax.experimental.pallas import tpu as pltpu
from jax.sharding import Mesh
from jax.sharding import PartitionSpec as P

MESH = pl.DeviceIdType.MESH
EP = ("z", "x", "core")
EPS = 1e-06
XN = 4
CN = 2
YN = 4
K3 = 3
CAP = YN * K3
CHUNKS = ((2, -2), (-5, 5), (7, -7), (4, -4), (8, 0), (1, -1), (-6, 6), (-3, 3))
ORDER = "00101213024312467124630254617325741603524670354673567575"

BF16 = jnp.bfloat16
F32 = jnp.float32


def chunks_of(zn):
    return CHUNKS if zn == 16 else tuple((d,) for d in range(zn))


def order_of(count):
    return [int(c) for c in ORDER] if count == 8 else [c for c in range(count) for _ in range(7)]


def kernel(
    zn,
    tokens_hbm,
    gain_hbm,
    ids_hbm,
    gates_hbm,
    w_gate,
    w_up,
    w_down,
    out,
    tokens,
    gain,
    ids,
    gates,
    t_sem,
    sbuf,
    xb,
    fb,
    xr,
    hb,
    wgv,
    wuv,
    wdv,
    pf,
    pb,
    rsb,
    gb,
    rb,
    ret,
    vb,
    wl_sem,
    ws_sem,
    wr_sem,
    ds_sem,
    dr_sem,
    ys_sem,
    yr_sem,
    xs_sem,
    xr_sem,
    hs_sem,
    hr_sem,
    rs_sem,
    rr_sem,
    os_sem,
    or_sem,
):
    zc, xc, cc, yc = (lax.axis_index(a) for a in ("z", "x", "core", "tp"))
    chunks = chunks_of(zn)
    offsets = [d for chunk in chunks for d in chunk]
    messages = 2 * len(offsets)
    starts = [0]
    for chunk in chunks:
        starts.append(starts[-1] + 2 * len(chunk))
    row_count, width = tokens_hbm.shape
    pieces = width // 128
    units = w_gate.shape[1]
    out_pieces = w_down.shape[1] // 128

    other_x = XN - 1 - xc
    pair_x = xc + 1 - 2 * lax.rem(xc, 2)
    up_y, down_y = lax.rem(yc + 1, YN), lax.rem(yc + YN - 1, YN)
    sibling = (zc, xc, 1 - cc, yc)
    pair = (zc, pair_x, cc, yc)
    sides = ((zc, xc, cc, up_y), (zc, xc, cc, down_y))

    def far(m, sign):
        d = offsets[m // 2] * sign
        return (lax.rem(zc + d + zn, zn), xc if m % 2 == 0 else other_x, 1 - cc, yc)

    small = ((tokens_hbm, tokens), (gain_hbm, gain), (ids_hbm, ids), (gates_hbm, gates))
    inputs = [pltpu.make_async_copy(src, dst, t_sem.at[i]) for i, (src, dst) in enumerate(small)]
    for copy in inputs:
        copy.start()
    barrier = pltpu.get_barrier_semaphore()
    greeted = [far(m, 1) for m in range(messages)] + [pair, *sides]
    for device in greeted:
        pl.semaphore_signal(barrier, inc=1, device_id=device, device_id_type=MESH)

    weights = ((w_gate, wgv), (w_up, wuv), (w_down, wdv))
    own_weights = [pltpu.make_async_copy(src, dst.at[0], wl_sem.at[i]) for i, (src, dst) in enumerate(weights)]
    for copy in own_weights:
        copy.start()

    for copy in inputs:
        copy.wait()
    wide = tokens[...].astype(F32)
    scale = lax.rsqrt(jnp.mean(wide * wide, axis=-1, keepdims=True) + EPS)
    normed = (wide * scale * gain[...]).astype(BF16)

    earlier = (
        lax.broadcasted_iota(jnp.int32, (row_count, row_count), 0)
        < lax.broadcasted_iota(jnp.int32, (row_count, row_count), 1)
    )
    earlier = jnp.where(earlier, 1.0, 0.0).astype(BF16)
    first_id, second_id = ids[0:1, :], ids[1:2, :]

    def expert_of(message):
        expert = jnp.zeros_like(message) - 1
        for m in range(messages):
            z, x, _, _ = far(m, 1)
            expert = jnp.where(message == m, z * (XN // 2) + x // 2, expert)
        return expert

    def selection(message, slot):
        expert = expert_of(message)
        hit_first, hit_second = first_id == expert, second_id == expert
        hit = jnp.where(hit_first | hit_second, 1.0, 0.0)
        rank = jnp.dot(hit.astype(BF16), earlier, preferred_element_type=F32)
        taken = jnp.where(rank == slot.astype(F32), hit, 0.0)
        return taken, hit_first

    line = lax.broadcasted_iota(jnp.int32, (128, 1), 0)
    taken, _ = selection(line // K3, K3 * yc + line % K3)
    sent_rows = messages * K3
    placed = jnp.dot(taken.astype(BF16), normed, preferred_element_type=F32)
    for i in range(pieces):
        fb[pl.ds(i, sent_rows, stride=pieces), :] = placed[:sent_rows, i * 128 : (i + 1) * 128]
    sbuf[...] = fb[0 : sent_rows * pieces, :].reshape(sent_rows, pieces, 128).astype(BF16)

    pl.semaphore_wait(barrier, len(greeted))

    def remote(src, dst, send_sem, recv_sem, device):
        copy = pltpu.make_async_remote_copy(
            src_ref=src, dst_ref=dst, send_sem=send_sem, recv_sem=recv_sem, device_id=device, device_id_type=MESH
        )
        copy.start()
        return copy

    def arrived(ref, sem):
        pltpu.make_async_copy(ref, ref, sem).wait()

    for c in range(len(chunks)):
        for m in range(starts[c], starts[c + 1]):
            rows = pl.ds(m * K3, K3)
            remote(sbuf.at[rows], xb.at[0, yc, rows], ds_sem, dr_sem.at[c], far(m, 1))
    shared_weights = [
        remote(src, dst.at[1], ws_sem.at[i], wr_sem.at[i], sibling) for i, (src, dst) in enumerate(weights)
    ]

    line = lax.broadcasted_iota(jnp.int32, (messages * CAP, 1), 0)
    taken, hit_first = selection(line // CAP, line % CAP)
    mix = jnp.transpose(taken * jnp.where(hit_first, gates[0:1, :], gates[1:2, :]))

    def run(c):
        m0, m1 = starts[c], starts[c + 1]
        return pl.ds(m0 * K3, (m1 - m0) * K3)

    def half(c, side):
        m0, m1 = starts[c], starts[c + 1]
        count = (m1 - m0) // 2 * K3
        return pl.ds(m0 * K3 + side * count, count)

    origin = [lax.rem(yc - r + YN, YN) for r in range(YN)]
    handles = {}

    def own_rows(c):
        block = xb.at[0, yc, run(c)]
        arrived(block, dr_sem.at[c])
        for part in (0, 1):
            for side in (0, 1):
                rows = xb.at[0, yc, half(c, (side + part) % 2)]
                handles["y", c, side, part] = remote(rows, rows, ys_sem, yr_sem.at[c, 2 * part + side], sides[side])
        handles["x", c, 0] = remote(block, xb.at[1, yc, run(c)], xs_sem, xr_sem.at[c], pair)

    def next_rows(c):
        for side in (0, 1):
            rel = 1 + 2 * side
            part = xb.at[0, origin[rel], half(c, side)]
            arrived(part, yr_sem.at[c, side])
            remote(part, part, ys_sem, yr_sem.at[c, 4], sides[side])
        for side in (0, 1):
            rel = 1 + 2 * side
            arrived(xb.at[0, origin[rel], half(c, 1 - side)], yr_sem.at[c, 2 + side])
            handles["x", c, rel] = remote(
                xb.at[0, origin[rel], run(c)],
                xb.at[1, origin[rel], run(c)],
                xs_sem,
                xr_sem.at[c],
                pair,
            )

    def last_rows(c):
        arrived(xb.at[0, origin[2], run(c)], yr_sem.at[c, 4])
        handles["x", c, 2] = remote(
            xb.at[0, origin[2], run(c)], xb.at[1, origin[2], run(c)], xs_sem, xr_sem.at[c], pair
        )

    def chunk_rows(c):
        count = 2 * CAP * (starts[c + 1] - starts[c])
        return 2 * CAP * starts[c], count

    def first_product(c):
        arrived(xb.at[1, :, run(c)], xr_sem.at[c])
        if not handles.get("weights"):
            handles["weights"] = True
            for copy in own_weights:
                copy.wait()
            for copy in shared_weights:
                copy.wait_recv()
        r0, count = chunk_rows(c)
        m0, m1 = starts[c], starts[c + 1]
        for side in (0, 1):
            for m in range(m0, m1):
                for y in range(YN):
                    at = ((side * (m1 - m0) + m - m0) * CAP + y * K3) * pieces
                    block = xb[side, y, m * K3 : (m + 1) * K3].astype(F32)
                    fb[at : at + K3 * pieces, :] = block.reshape(K3 * pieces, 128)
        for i in range(pieces):
            xr[0:count, i * 128 : (i + 1) * 128] = fb[pl.ds(i, count, stride=pieces), :].astype(BF16)
        for core in range(CN):
            gate = jnp.dot(xr[0:count, :], wgv[core], preferred_element_type=F32)
            upper = jnp.dot(xr[0:count, :], wuv[core], preferred_element_type=F32)
            hidden = gate / (1.0 + jnp.exp(-gate)) * upper
            hb[0, core, r0 : r0 + count, :] = hidden.astype(BF16)
            give_hidden(c, core, core)
        for side in (0, 1):
            give_hidden(c, side, 1 - side)

    def hidden_rows(c, rel, core):
        r0, count = chunk_rows(c)
        return hb.at[rel, core, pl.ds(r0, count)]

    def give_hidden(c, side, core):
        sem = hr_sem.at[c, side if core == side else 2 + side]
        remote(hidden_rows(c, 0, core), hidden_rows(c, 1 + 2 * side, core), hs_sem, sem, sides[side])

    def next_hidden(c):
        for side in (0, 1):
            block = hidden_rows(c, 1 + 2 * side, side)
            arrived(block, hr_sem.at[c, side])
            remote(block, hidden_rows(c, 2, side), hs_sem, hr_sem.at[c, 4], sides[side])

    def second_product(c):
        r0, count = chunk_rows(c)
        for side in (0, 1):
            arrived(hidden_rows(c, 1 + 2 * side, 1 - side), hr_sem.at[c, 2 + side])
        arrived(hb.at[2, :, pl.ds(r0, count)], hr_sem.at[c, 4])
        total = None
        for rel in range(YN):
            first = pl.multiple_of(origin[rel] * units, units)
            for core in range(CN):
                term = jnp.dot(
                    hb[rel, core, r0 : r0 + count, :],
                    wdv[core, pl.ds(first, units), :],
                    preferred_element_type=F32,
                )
                total = term if total is None else total + term
        at, part = r0 // 2, count // 2
        pf[at : at + part, :] = total[0:part]
        pb[at : at + part, :] = total[part:count].astype(BF16)
        handles["r", c] = remote(
            pb.at[pl.ds(at, part)], rsb.at[pl.ds(at, part)], rs_sem, rr_sem.at[c], pair
        )

    def give_back(c):
        handles["r", c].wait_recv()
        r0, count = chunk_rows(c)
        at, part = r0 // 2, count // 2
        total = pf[at : at + part, :] + rsb[at : at + part, :].astype(F32)
        for i in range(out_pieces):
            gb[pl.ds(i, part, stride=out_pieces), :] = total[:, i * 128 : (i + 1) * 128]
        rb[at * out_pieces : (at + part) * out_pieces, :] = gb[0 : part * out_pieces, :].astype(BF16)
        size = CAP * out_pieces
        for m in range(starts[c], starts[c + 1]):
            rows = pl.ds(m * size, size)
            remote(rb.at[rows], ret.at[rows], os_sem, or_sem, far(m, -1))

    stages = (own_rows, next_rows, last_rows, first_product, next_hidden, second_product, give_back)
    reached = [0] * len(chunks)
    for c in order_of(len(chunks)):
        stages[reached[c]](c)
        reached[c] += 1

    size = CAP * out_pieces
    arrived(ret, or_sem)
    gb[0 : messages * size, :] = ret[...].astype(F32)
    for i in range(out_pieces):
        vb[:, i * 128 : (i + 1) * 128] = gb[pl.ds(i, messages * CAP, stride=out_pieces), :].astype(BF16)
    values = vb[...]
    high = mix.astype(BF16)
    rest = mix - high.astype(F32)
    middle = rest.astype(BF16)
    low = (rest - middle.astype(F32)).astype(BF16)
    mixed = jnp.dot(high, values, preferred_element_type=F32)
    mixed = mixed + jnp.dot(middle, values, preferred_element_type=F32)
    mixed = mixed + jnp.dot(low, values, preferred_element_type=F32)
    out[...] = mixed.astype(BF16)

    for copy in shared_weights:
        copy.wait_send()
    three = pl.ds(0, YN - 1)
    for ref, sem in (
        (sbuf, ds_sem),
        (xb.at[0, three], ys_sem),
        (xb.at[1], xs_sem),
        (hb.at[three], hs_sem),
        (pb, rs_sem),
        (rb, os_sem),
    ):
        arrived(ref, sem)


def on_device(zn, tokens, norm_gain, expert_ids, gate_weights, w_gate, w_up, w_down):
    chunks = chunks_of(zn)
    n = len(chunks)
    messages = 2 * sum(len(chunk) for chunk in chunks)
    most = 2 * max(len(chunk) for chunk in chunks)
    row_count, width = tokens.shape
    pieces = width // 128
    units = w_gate.shape[1]
    block, columns = w_down.shape
    out_pieces = columns // 128
    rows = messages * CAP
    dma = pltpu.SemaphoreType.DMA
    scratch = [
        pltpu.VMEM((row_count, width), BF16),
        pltpu.VMEM((1, width), F32),
        pltpu.VMEM((2, row_count), jnp.int32),
        pltpu.VMEM((2, row_count), F32),
        dma((4,)),
        pltpu.VMEM((messages * K3, pieces, 128), BF16),
        pltpu.VMEM((2, YN, messages * K3, pieces, 128), BF16),
        pltpu.VMEM((max(2 * most * CAP, messages * K3) * pieces + pieces, 128), F32),
        pltpu.VMEM((2 * most * CAP, width), BF16),
        pltpu.VMEM((YN, CN, 2 * rows, units), BF16),
        pltpu.VMEM((CN, width, units), BF16),
        pltpu.VMEM((CN, width, units), BF16),
        pltpu.VMEM((CN, block, columns), BF16),
        pltpu.VMEM((rows, columns), F32),
        pltpu.VMEM((rows, columns), BF16),
        pltpu.VMEM((rows, columns), BF16),
        pltpu.VMEM((rows * out_pieces + 8, 128), F32),
        pltpu.VMEM((rows * out_pieces, 128), BF16),
        pltpu.VMEM((rows * out_pieces, 128), BF16),
        pltpu.VMEM((rows, columns), BF16),
        dma((3,)),
        dma((3,)),
        dma((3,)),
        dma(()),
        dma((n,)),
        dma(()),
        dma((n, 5)),
        dma(()),
        dma((n,)),
        dma(()),
        dma((n, 5)),
        dma(()),
        dma((n,)),
        dma(()),
        dma(()),
    ]
    vmem = pl.BlockSpec(memory_space=pltpu.VMEM)
    hbm = pl.BlockSpec(memory_space=pl.ANY)
    return pl.pallas_call(
        functools.partial(kernel, zn),
        out_shape=jax.ShapeDtypeStruct((row_count, columns), BF16),
        in_specs=[hbm] * 7,
        out_specs=vmem,
        scratch_shapes=scratch,
        compiler_params=pltpu.CompilerParams(
            collective_id=0, has_side_effects=True, vmem_limit_bytes=60 * 1024 * 1024
        ),
        name="expert_layer",
    )(tokens, norm_gain.reshape(1, width), expert_ids.T, gate_weights.T, w_gate, w_up, w_down)


def solution(mesh):
    zn = mesh.shape["ep"] // (XN * CN)
    finer = Mesh(mesh.devices.reshape(zn, XN, CN, mesh.shape["tp"]), (*EP, "tp"))
    placed = (
        P(EP, None),
        P(),
        P(EP, None),
        P(EP, None),
        P(None, (*EP, "tp")),
        P(None, (*EP, "tp")),
        P(EP, "tp"),
    )
    return jax.shard_map(
        functools.partial(on_device, zn), mesh=finer, in_specs=placed, out_specs=P(EP, "tp"), check_vma=False
    )
```
